32 devices in a mesh: grp: 2 (over y), sp: 4 (over z), tp: 4 (over x, core).
Axes of the slice: x: 2, y: 2, z: 4, core: 2. Of those that a mesh axis runs over, the one named last changes fastest.
Arguments:
- target: bfloat16 [1024, 2048], P(('grp', 'sp', 'tp')), parts along dimension 0, may hold values from -6 to 6
- source: bfloat16 [8192, 2048], P(('grp', 'sp', 'tp')), parts along dimension 0, may hold values from -6 to 6
- norm_gain: float32 [2048], replicated, may hold values from 0.1 to 1.9
- query_weight: bfloat16 [2048, 2048], P(None, 'tp'), may hold values from -0.125 to 0.125
- key_weight: bfloat16 [2048, 256], replicated, may hold values from -0.125 to 0.125
- value_weight: bfloat16 [2048, 256], replicated, may hold values from -0.125 to 0.125
- output_weight: bfloat16 [2048, 2048], P('tp'), may hold values from -0.125 to 0.125
- saved_out: bfloat16 [1024, 2048], P(('grp', 'sp'), 'tp'), parts along dimension 0, may hold values from -3 to 3
- log_shift: float32 [16, 1024], P('tp', ('grp', 'sp')), parts along dimension 1, may hold values from 0 to 2
- out_grad: bfloat16 [1024, 2048], P(('grp', 'sp', 'tp')), parts along dimension 0, may hold values from -48 to 48
Outputs:
- target_grad: float32 [1024, 2048], P(('grp', 'sp', 'tp')), parts along dimension 0
- source_grad: float32 [8192, 2048], P(('grp', 'sp', 'tp')), parts along dimension 0
- query_weight_grad: float32 [4096, 2048], P(('grp', 'sp'), 'tp'), parts along dimension 0
The draws below stay inside these ranges and needn't reach their ends.
There are 2 independent parts, one for each index of `grp`. The reference program is written for one: setup_inputs(seed, part) draws one part's arguments, and reference() takes and returns one part's arrays. A program takes and returns all parts, laid end to end along the dimension named above; an argument that names none is the same for every part. Nothing has to cross between parts.
All inputs are finite; a program needn't handle non-finite values.
Results may differ from the reference program's by a relative error of at most 0.02.
Values may be sent and summed in bfloat16 or wider, within the bound.
No kernel may reach another device: no remote copies, remote signals or barrier semaphores. Data moves between devices by JAX's collectives and lax.ppermute only.
A program may use at most 64 MiB of HBM per device.

```python
import jax
import jax.numpy as jnp
from jax import lax

D = 2048
HEADS = 16
HEAD_DIM = 128
KV_HEADS = 2
SRC = 4096
TGT = 512


def shard_levels(stream_key, extent, shards, low, top_value):
    def one(axis_at, shards_of):
        steps = jax.random.uniform(jax.random.fold_in(jax.random.fold_in(stream_key, 6), axis_at), (shards_of,), jnp.float32, low / len(shards), top_value / len(shards))
        return jnp.repeat(jnp.exp(steps), extent[axis_at] // shards_of).reshape((-1,) + (1,) * (len(extent) - axis_at - 1))

    gain = one(*shards[0])
    for cut in shards[1:]:
        gain = gain * one(*cut)
    return gain


def centred(rng, shape, spread, reach, pieces=(), kind=jnp.bfloat16):
    loudness = shard_levels(rng, shape, pieces, -0.22, 0.18) if pieces else 1.0
    entries = jax.random.normal(rng, shape, jnp.float32) * spread * loudness
    return jnp.minimum(jnp.maximum(entries, -reach), reach).astype(kind)


def setup_inputs(seed: int = 0, part: int = 0) -> dict:
    splits = jax.random.split(jax.random.key(seed), 11)
    part_splits = jax.random.split(jax.random.fold_in(splits[10], part), 11)
    target = centred(part_splits[0], (TGT, D), 1.0, 6.0, ((0, 16),))
    source = centred(part_splits[1], (SRC, D), 1.0, 6.0, ((0, 16),))
    norm_gain = jnp.clip(1.0 + 0.18 * jax.random.normal(splits[2], (D,), jnp.float32), 0.1, 1.9)
    query_weight = centred(splits[3], (D, HEADS * HEAD_DIM), D ** -0.5, 0.125, ((1, 4),))
    key_weight = centred(splits[4], (D, KV_HEADS * HEAD_DIM), D ** -0.5, 0.125)
    value_weight = centred(splits[5], (D, KV_HEADS * HEAD_DIM), D ** -0.5, 0.125)
    output_weight = centred(splits[6], (HEADS * HEAD_DIM, D), (HEADS * HEAD_DIM) ** -0.5, 0.125, ((0, 4),))
    saved_out = centred(part_splits[7], (TGT, HEADS * HEAD_DIM), 0.5, 3.0, ((0, 4), (1, 4)))
    log_shift = jnp.clip(2.0 * jax.random.uniform(part_splits[8], (HEADS, TGT), jnp.float32) ** shard_levels(part_splits[8], (HEADS, TGT), ((0, 4), (1, 4)), -0.2, 0.2), 0.0, 2.0)
    out_grad = centred(part_splits[9], (TGT, D), 8.0, 48.0, ((0, 16),))
    return dict(target=target, source=source, norm_gain=norm_gain, query_weight=query_weight, key_weight=key_weight, value_weight=value_weight, output_weight=output_weight, saved_out=saved_out, log_shift=log_shift, out_grad=out_grad)


def reference(target, source, norm_gain, query_weight, key_weight, value_weight, output_weight, saved_out, log_shift, out_grad):
    group_size = HEADS // KV_HEADS
    factor = HEAD_DIM ** (-0.5)
    offset = jnp.log(jnp.float32(SRC))
    target_wide = target.astype(jnp.float32)
    root_mean = jnp.sqrt(lax.optimization_barrier(jnp.mean(target_wide * target_wide, axis=1, keepdims=True)) + 1e-06)
    normed = (target_wide / root_mean * norm_gain).astype(jnp.bfloat16)
    queries = jnp.dot(normed, query_weight, preferred_element_type=jnp.float32).astype(jnp.bfloat16)
    key_rows = jnp.dot(source, key_weight, preferred_element_type=jnp.float32).astype(jnp.bfloat16)
    values = jnp.dot(source, value_weight, preferred_element_type=jnp.float32).astype(jnp.bfloat16)
    out_back = jnp.dot(out_grad, output_weight.T, preferred_element_type=jnp.float32).astype(jnp.bfloat16)
    products = out_back.astype(jnp.float32) * saved_out.astype(jnp.float32)
    drop_term = lax.optimization_barrier(jnp.sum(products.reshape(TGT, HEADS, HEAD_DIM), axis=2))

    def one_head(head_id):
        pair_index = head_id // group_size
        query_head = lax.dynamic_slice_in_dim(queries, head_id * HEAD_DIM, HEAD_DIM, 1)
        back_head = lax.dynamic_slice_in_dim(out_back, head_id * HEAD_DIM, HEAD_DIM, 1)
        key_head = lax.dynamic_slice_in_dim(key_rows, pair_index * HEAD_DIM, HEAD_DIM, 1)
        value_head = lax.dynamic_slice_in_dim(values, pair_index * HEAD_DIM, HEAD_DIM, 1)
        shift_row = lax.dynamic_index_in_dim(log_shift, head_id, 0, keepdims=False)
        drop_row = lax.dynamic_index_in_dim(drop_term, head_id, 1, keepdims=False)
        scores = jnp.dot(query_head, key_head.T, preferred_element_type=jnp.float32) * factor
        prob = jnp.exp(scores - shift_row[:, None] - offset)
        prob_grad = jnp.dot(back_head, value_head.T, preferred_element_type=jnp.float32)
        score_grad = (prob * (prob_grad - drop_row[:, None]) * factor).astype(jnp.bfloat16)
        prob_low = prob.astype(jnp.bfloat16)
        query_part = jnp.dot(score_grad, key_head, preferred_element_type=jnp.float32)
        key_part = jnp.dot(score_grad.T, query_head, preferred_element_type=jnp.float32)
        value_part = jnp.dot(prob_low.T, back_head, preferred_element_type=jnp.float32)
        return (query_part, key_part, value_part)
    head_ids = jnp.arange(HEADS, dtype=jnp.int32)
    query_all, key_all, value_all = lax.map(one_head, head_ids)
    query_grad = jnp.transpose(query_all, (1, 0, 2)).reshape(TGT, HEADS * HEAD_DIM).astype(jnp.bfloat16)
    key_sum = lax.optimization_barrier(jnp.sum(key_all.reshape(KV_HEADS, group_size, SRC, HEAD_DIM), axis=1))
    value_sum = lax.optimization_barrier(jnp.sum(value_all.reshape(KV_HEADS, group_size, SRC, HEAD_DIM), axis=1))
    key_grad = jnp.transpose(key_sum, (1, 0, 2)).reshape(SRC, KV_HEADS * HEAD_DIM).astype(jnp.bfloat16)
    value_grad = jnp.transpose(value_sum, (1, 0, 2)).reshape(SRC, KV_HEADS * HEAD_DIM).astype(jnp.bfloat16)
    source_grad = jnp.dot(key_grad, key_weight.T, preferred_element_type=jnp.float32) + jnp.dot(value_grad, value_weight.T, preferred_element_type=jnp.float32)
    normed_grad = jnp.dot(query_grad, query_weight.T, preferred_element_type=jnp.float32)
    scaled_grad = normed_grad * norm_gain
    target_grad = scaled_grad / root_mean - target_wide * lax.optimization_barrier(jnp.mean(scaled_grad * target_wide, axis=1, keepdims=True)) / root_mean ** 3
    query_weight_grad = jnp.dot(normed.T, query_grad, preferred_element_type=jnp.float32)
    return (target_grad, source_grad, query_weight_grad)
```

```python
import math

import jax
import jax.numpy as jnp
from jax import lax
from jax.experimental import pallas as pl
from jax.experimental.pallas import tpu as pltpu
from jax.sharding import PartitionSpec as P

HEADS = 16
HEAD_DIM = 128
KV_HEADS = 2
LOG2E = math.log2(math.e)
FACTOR = HEAD_DIM ** (-0.5)
BF16 = jnp.bfloat16
F32 = jnp.float32


def dot(a, b, dims):
    return lax.dot_general(a, b, (dims, ((), ())), preferred_element_type=F32)


def project_kernel(
    target_ref, back_ref, gain_ref, wq_ref, wo_ref, saved_ref, query_ref, out_ref, drop_ref, normed_ref
):
    head = pl.program_id(0)

    @pl.when(head == 0)
    def _():
        wide = target_ref[...].astype(F32)
        root = jnp.sqrt(jnp.mean(wide * wide, axis=1, keepdims=True) + 1e-06)
        normed_ref[...] = (wide / root * gain_ref[...]).astype(BF16)

    query_ref[...] = dot(normed_ref[...], wq_ref[...], ((1,), (0,))).astype(BF16)
    back = dot(back_ref[...], wo_ref[...], ((1,), (1,))).astype(BF16)
    out_ref[...] = back
    products = back.astype(F32) * saved_ref[...].astype(F32)
    ones = jnp.ones((8, HEAD_DIM), F32)
    sums = lax.dot_general(
        ones,
        products,
        (((1,), (1,)), ((), ())),
        preferred_element_type=F32,
        precision=lax.Precision.HIGHEST,
    )
    drop_ref[pl.ds(head, 1), :] = sums[:1]


def project(target, back, gain, wq, wo, saved):
    rows, width = target.shape
    heads = wq.shape[1] // HEAD_DIM
    column = pl.BlockSpec((rows, HEAD_DIM), lambda h: (0, h))
    return pl.pallas_call(
        project_kernel,
        grid=(heads,),
        in_specs=[
            pl.BlockSpec((rows, width), lambda h: (0, 0)),
            pl.BlockSpec((rows, width), lambda h: (0, 0)),
            pl.BlockSpec((1, width), lambda h: (0, 0)),
            pl.BlockSpec((width, HEAD_DIM), lambda h: (0, h)),
            pl.BlockSpec((HEAD_DIM, width), lambda h: (h, 0)),
            column,
        ],
        out_specs=[column, column, pl.BlockSpec((heads, rows), lambda h: (0, 0))],
        out_shape=[
            jax.ShapeDtypeStruct((rows, heads * HEAD_DIM), BF16),
            jax.ShapeDtypeStruct((rows, heads * HEAD_DIM), BF16),
            jax.ShapeDtypeStruct((heads, rows), F32),
        ],
        scratch_shapes=[pltpu.VMEM((rows, width), BF16)],
        name="project",
    )(target, back, gain.reshape(1, width), wq, wo, saved)


def attend(query, back, shift, drop, pairs, grads, offset):
    rows = query.shape[0]
    heads = query.shape[1] // HEAD_DIM
    source_rows = pairs.shape[0]
    tile = min(source_rows, 256)
    first = grads is None

    def kernel(query_ref, back_ref, shift_ref, drop_ref, pairs_ref, *rest):
        (grads_in,) = (None,) if first else rest[:1]
        part_ref, grads_ref = rest[-2:]
        parts = [slice(h * HEAD_DIM, (h + 1) * HEAD_DIM) for h in range(heads)]
        queries = jnp.concatenate([query_ref[:, p] for p in parts], axis=0)
        backs = jnp.concatenate([back_ref[:, p] for p in parts], axis=0)
        line = lambda ref: jnp.concatenate([ref[h : h + 1, :] for h in range(heads)], axis=1)
        shifts = (line(shift_ref) + offset) * LOG2E
        drops = line(drop_ref)
        total = None
        for at in range(0, source_rows, tile):
            span = slice(at, at + tile)
            keys = pairs_ref[span, :HEAD_DIM]
            values = pairs_ref[span, HEAD_DIM:]
            scores = dot(keys, queries, ((1,), (1,)))
            prob = jnp.exp2(scores * (FACTOR * LOG2E) - shifts)
            prob_grad = dot(values, backs, ((1,), (1,)))
            score_grad = (prob * (prob_grad - drops) * FACTOR).astype(BF16)
            key_part = dot(score_grad, queries, ((1,), (0,)))
            value_part = dot(prob.astype(BF16), backs, ((1,), (0,)))
            if not first:
                key_part = key_part + grads_in[span, :HEAD_DIM]
                value_part = value_part + grads_in[span, HEAD_DIM:]
            grads_ref[span, :HEAD_DIM] = key_part
            grads_ref[span, HEAD_DIM:] = value_part
            share = dot(score_grad, keys, ((0,), (0,)))
            total = share if total is None else total + share
        for h, p in enumerate(parts):
            part_ref[:, p] = total[h * rows : (h + 1) * rows].astype(BF16)

    operands = (query, back, shift, drop, pairs) + (() if first else (grads,))
    return pl.pallas_call(
        kernel,
        out_shape=[
            jax.ShapeDtypeStruct((rows, heads * HEAD_DIM), BF16),
            jax.ShapeDtypeStruct((source_rows, 2 * HEAD_DIM), F32),
        ],
        input_output_aliases={} if first else {5: 1},
        name="attend",
    )(*operands)


def shards(
    target,
    source,
    norm_gain,
    query_weight,
    key_weight,
    value_weight,
    output_weight,
    saved_out,
    log_shift,
    out_grad,
):
    tp_count = lax.axis_size("tp")
    sp_count = lax.axis_size("sp")
    local_heads = query_weight.shape[1] // HEAD_DIM
    group_size = HEADS // KV_HEADS
    inner = 2 if tp_count % 2 == 0 and group_size % (2 * local_heads) == 0 else 1
    outer = tp_count // inner
    tp_at = lax.axis_index("tp")
    sp_at = lax.axis_index("sp")
    outer_at, inner_at = tp_at // inner, tp_at % inner
    offset = math.log(source.shape[0] * tp_count * sp_count)
    own_rows, model_width = target.shape

    def to_outer(x, d):
        pairs = [
            (o * inner + c, (o + d) % outer * inner + c) for o in range(outer) for c in range(inner)
        ]
        return lax.ppermute(x, "tp", pairs)

    def to_inner(x, e):
        pairs = [
            (o * inner + c, o * inner + (c + e) % inner) for o in range(outer) for c in range(inner)
        ]
        return lax.ppermute(x, "tp", pairs)

    def to_sp(x, d):
        return lax.ppermute(x, "sp", [(i, (i + d) % sp_count) for i in range(sp_count)])

    def owner(d, e):
        return (outer_at - d) % outer * inner + (inner_at - e) % inner

    def tp_pieces(x):
        line = [x] + [to_outer(x, d) for d in range(1, outer)]
        pieces = [(owner(d, 0), piece) for d, piece in enumerate(line)]
        for e in range(1, inner):
            pieces += [(owner(d, e), to_inner(piece, e)) for d, piece in enumerate(line)]
        return pieces

    def placed(pieces, count):
        size = pieces[0][1].shape[0]
        whole = jnp.zeros((count * size,) + pieces[0][1].shape[1:], pieces[0][1].dtype)
        for at, piece in pieces:
            whole = lax.dynamic_update_slice_in_dim(whole, piece, at * size, 0)
        return whole

    target_all = placed(tp_pieces(target), tp_count)
    back_all = placed(tp_pieces(out_grad), tp_count)
    shifts = [log_shift] + [to_sp(log_shift, d) for d in range(1, sp_count)]

    target_wide = target.astype(F32)
    root_mean = jnp.sqrt(jnp.mean(target_wide * target_wide, axis=1, keepdims=True) + 1e-06)
    normed = (target_wide / root_mean * norm_gain).astype(BF16)
    block_width = model_width // sp_count

    def normed_block(at):
        return lax.dynamic_slice_in_dim(normed, at % sp_count * block_width, block_width, 1)

    normed_cols = placed(
        [(sp_at, normed_block(sp_at))]
        + [
            ((sp_at - d) % sp_count, to_sp(normed_block(sp_at + d), d)) for d in range(1, sp_count)
        ],
        sp_count,
    )

    keys = dot(source, key_weight, ((1,), (0,))).astype(BF16)
    values = dot(source, value_weight, ((1,), (0,))).astype(BF16)

    def pair_of(at):
        return at % outer * inner * local_heads // group_size

    def pair_cols(at):
        start = pair_of(at) * HEAD_DIM
        return jnp.concatenate(
            [lax.dynamic_slice_in_dim(x, start, HEAD_DIM, 1) for x in (keys, values)], axis=1
        )

    line = [pair_cols(outer_at)] + [
        to_outer(pair_cols(outer_at + d), d) for d in range(1, outer)
    ]
    pairs = jnp.concatenate(
        line + [to_inner(piece, e) for e in range(1, inner) for piece in line], axis=0
    )

    query, back, drop = project(
        target_all, back_all, norm_gain, query_weight, output_weight, saved_out
    )
    grads = None
    query_sum = None
    for d in range(sp_count):
        if d + 1 < sp_count:
            following = tuple(to_sp(x, 1) for x in (query, back, drop))
        part, grads = attend(query, back, shifts[d], drop, pairs, grads, offset)
        if d:
            part = to_sp(part, sp_count - d)
        query_sum = part.astype(F32) if query_sum is None else query_sum + part.astype(F32)
        query, back, drop = following
    query_grad = query_sum.astype(BF16)

    gathered = placed(
        [(sp_at, query_grad)]
        + [((sp_at - d) % sp_count, to_sp(query_grad, d)) for d in range(1, sp_count)],
        sp_count,
    )

    partial = dot(query_grad, query_weight, ((1,), (1,))).astype(BF16)

    def rows_of(at):
        return lax.dynamic_slice_in_dim(partial, at * own_rows, own_rows, 0)

    line = []
    for d in range(outer):
        piece = rows_of(owner(d, 0)).astype(F32)
        for e in range(1, inner):
            piece = piece + to_inner(rows_of(owner(d, e)), inner - e).astype(F32)
        line.append(piece)
    normed_grad = line[0]
    for d in range(1, outer):
        normed_grad = normed_grad + to_outer(line[d].astype(BF16), outer - d).astype(F32)

    scaled_grad = normed_grad * norm_gain
    target_grad = (
        scaled_grad / root_mean
        - target_wide * jnp.mean(scaled_grad * target_wide, axis=1, keepdims=True) / root_mean**3
    )

    count = source.shape[0]
    blocks = [[None] * outer for _ in range(inner)]
    for e in range(inner):
        for d in range(outer):
            at = (e * outer + d) * count
            blocks[e][d] = grads[at : at + count]
    combined = []
    for d in range(outer):
        piece = blocks[0][d]
        for e in range(1, inner):
            piece = piece + to_inner(blocks[e][d].astype(BF16), inner - e).astype(F32)
        piece = piece.astype(BF16)
        combined.append((pair_of(outer_at + d), to_outer(piece, outer - d) if d else piece))
    source_grad = None
    key_cols, value_cols = [], []
    for p in range(KV_HEADS):
        total = None
        for at, piece in combined:
            piece = jnp.where(at == p, piece.astype(F32), 0.0)
            total = piece if total is None else total + piece
        total = total.astype(BF16)
        key_cols.append(total[:, :HEAD_DIM])
        value_cols.append(total[:, HEAD_DIM:])
    source_grad = dot(jnp.concatenate(key_cols, axis=1), key_weight, ((1,), (1,))) + dot(
        jnp.concatenate(value_cols, axis=1), value_weight, ((1,), (1,))
    )

    normed_rows = jnp.zeros((sp_count, tp_count, own_rows, block_width), BF16)
    for at, piece in tp_pieces(normed_cols):
        piece = piece.reshape(sp_count, 1, own_rows, block_width)
        normed_rows = lax.dynamic_update_slice_in_dim(normed_rows, piece, at, 1)
    query_weight_grad = dot(
        normed_rows.reshape(sp_count * tp_count * own_rows, block_width), gathered, ((0,), (0,))
    )
    return (target_grad, source_grad, query_weight_grad)


def solution(mesh):
    return jax.shard_map(
        shards,
        mesh=mesh,
        in_specs=(
            P(("grp", "sp", "tp"), None),
            P(("grp", "sp", "tp"), None),
            P(),
            P(None, "tp"),
            P(),
            P(),
            P("tp", None),
            P(("grp", "sp"), "tp"),
            P("tp", ("grp", "sp")),
            P(("grp", "sp", "tp"), None),
        ),
        out_specs=(
            P(("grp", "sp", "tp"), None),
            P(("grp", "sp", "tp"), None),
            P(("grp", "sp"), "tp"),
        ),
        check_vma=False,
    )
```

```python
import math

import jax
import jax.numpy as jnp
from jax import lax
from jax.experimental import pallas as pl
from jax.experimental.pallas import tpu as pltpu
from jax.sharding import PartitionSpec as P

HEADS = 16
HEAD_DIM = 128
KV_HEADS = 2
LOG2E = math.log2(math.e)
FACTOR = HEAD_DIM ** (-0.5)
BF16 = jnp.bfloat16
F32 = jnp.float32


def dot(a, b, dims):
    return lax.dot_general(a, b, (dims, ((), ())), preferred_element_type=F32)


def vmem(count):
    return [pl.BlockSpec(memory_space=pltpu.VMEM) for _ in range(count)]


def project_kernel(
    target_ref, back_ref, gain_ref, wq_ref, wo_ref, saved_ref, shift_ref, message_ref
):
    rows = target_ref.shape[0]
    width = wq_ref.shape[1]
    heads = width // HEAD_DIM
    wide = target_ref[...].astype(F32)
    root = jnp.sqrt(jnp.mean(wide * wide, axis=1, keepdims=True) + 1e-06)
    normed = (wide / root * gain_ref[...]).astype(BF16)
    message_ref[:rows, :width] = dot(normed, wq_ref[...], ((1,), (0,))).astype(BF16)
    back = dot(back_ref[...], wo_ref[...], ((1,), (1,))).astype(BF16)
    message_ref[:rows, width:] = back
    products = back.astype(F32) * saved_ref[...].astype(F32)
    ones = jnp.ones((8, HEAD_DIM), F32)
    drops = [
        lax.dot_general(
            ones,
            products[:, h * HEAD_DIM : (h + 1) * HEAD_DIM],
            (((1,), (1,)), ((), ())),
            preferred_element_type=F32,
            precision=lax.Precision.HIGHEST,
        )[:1]
        for h in range(heads)
    ]
    stats = jnp.concatenate([shift_ref[...]] + drops, axis=0)
    high = stats.astype(BF16).astype(F32)
    stats = jnp.concatenate([high, stats - high], axis=0)
    extra = message_ref.shape[0] - rows
    if extra > 4 * heads:
        stats = jnp.concatenate([stats, jnp.zeros((extra - 4 * heads, rows), F32)], axis=0)
    message_ref[rows:, :rows] = stats.astype(BF16)
    if rows < message_ref.shape[1]:
        message_ref[rows:, rows:] = jnp.zeros((extra, message_ref.shape[1] - rows), BF16)


def project(target, back, gain, wq, wo, saved, shift):
    rows, width = target.shape
    heads = wq.shape[1] // HEAD_DIM
    extra = -(-4 * heads // 16) * 16
    return pl.pallas_call(
        project_kernel,
        in_specs=vmem(7),
        out_specs=vmem(1)[0],
        out_shape=jax.ShapeDtypeStruct((rows + extra, 2 * heads * HEAD_DIM), BF16),
        name="project",
    )(target, back, gain.reshape(1, width), wq, wo, saved, shift)


def attend(message, pairs, grads, offset, heads, rows, kept=None):
    source_rows = pairs.shape[0]
    tile = min(source_rows, 256)
    first = grads is None
    last = kept is not None
    width = heads * HEAD_DIM

    def kernel(message_ref, pairs_ref, *rest):
        grads_in = None if first else rest[0]
        outs = rest[0 if first else 1 :]
        part_ref = outs[0]
        parts = [slice(h * HEAD_DIM, (h + 1) * HEAD_DIM) for h in range(heads)]
        queries = jnp.concatenate([message_ref[:rows, p] for p in parts], axis=0)
        backs = jnp.concatenate(
            [message_ref[:rows, width + p.start : width + p.stop] for p in parts], axis=0
        )
        stats = message_ref[rows:, :rows].astype(F32)
        stats = stats[: 2 * heads] + stats[2 * heads : 4 * heads]
        line = lambda at: jnp.concatenate([stats[at + h : at + h + 1] for h in range(heads)], axis=1)
        shifts = (line(0) + offset) * LOG2E
        drops = line(heads)
        total = None
        for at in range(0, source_rows, tile):
            span = slice(at, at + tile)
            keys = pairs_ref[span, :HEAD_DIM]
            values = pairs_ref[span, HEAD_DIM:]
            scores = dot(keys, queries, ((1,), (1,)))
            prob = jnp.exp2(scores * (FACTOR * LOG2E) - shifts)
            prob_grad = dot(values, backs, ((1,), (1,)))
            score_grad = (prob * (prob_grad - drops) * FACTOR).astype(BF16)
            key_part = dot(score_grad, queries, ((1,), (0,)))
            value_part = dot(prob.astype(BF16), backs, ((1,), (0,)))
            if not first:
                key_part = key_part + grads_in[span, :HEAD_DIM]
                value_part = value_part + grads_in[span, HEAD_DIM:]
            if last and at >= kept:
                to, place = outs[2], slice(at - kept, at - kept + tile)
            else:
                to, place = outs[1], span
            to[place, :HEAD_DIM] = key_part.astype(to.dtype)
            to[place, HEAD_DIM:] = value_part.astype(to.dtype)
            share = dot(score_grad, keys, ((0,), (0,)))
            total = share if total is None else total + share
        for h, p in enumerate(parts):
            part_ref[:, p] = total[h * rows : (h + 1) * rows].astype(BF16)

    held = kept if last else source_rows
    shapes = [
        jax.ShapeDtypeStruct((rows, width), BF16),
        jax.ShapeDtypeStruct((held, 2 * HEAD_DIM), F32),
    ]
    if last and kept < source_rows:
        shapes.append(jax.ShapeDtypeStruct((source_rows - kept, 2 * HEAD_DIM), BF16))
    operands = (message, pairs) + (() if first else (grads,))
    return pl.pallas_call(
        kernel,
        in_specs=vmem(len(operands)),
        out_specs=vmem(len(shapes)),
        out_shape=shapes,
        input_output_aliases={} if first or last else {2: 1},
        cost_estimate=pl.CostEstimate(
            flops=10 * rows * width * source_rows,
            transcendentals=rows * heads * source_rows,
            bytes_accessed=8 * source_rows * width,
        ),
        name="attend",
    )(*operands)


def shards(
    target,
    source,
    norm_gain,
    query_weight,
    key_weight,
    value_weight,
    output_weight,
    saved_out,
    log_shift,
    out_grad,
):
    tp_count = lax.axis_size("tp")
    sp_count = lax.axis_size("sp")
    local_heads = query_weight.shape[1] // HEAD_DIM
    group_size = HEADS // KV_HEADS
    inner = 2 if tp_count % 2 == 0 and group_size % (2 * local_heads) == 0 else 1
    outer = tp_count // inner
    tp_at = lax.axis_index("tp")
    sp_at = lax.axis_index("sp")
    outer_at, inner_at = tp_at // inner, tp_at % inner
    offset = math.log(source.shape[0] * tp_count * sp_count)
    own_rows, model_width = target.shape

    def to_outer(x, d):
        pairs = [
            (o * inner + c, (o + d) % outer * inner + c) for o in range(outer) for c in range(inner)
        ]
        return lax.ppermute(x, "tp", pairs)

    def to_inner(x, e):
        pairs = [
            (o * inner + c, o * inner + (c + e) % inner) for o in range(outer) for c in range(inner)
        ]
        return lax.ppermute(x, "tp", pairs)

    def to_sp(x, d):
        return lax.ppermute(x, "sp", [(i, (i + d) % sp_count) for i in range(sp_count)])

    def owner(d, e):
        return (outer_at - d) % outer * inner + (inner_at - e) % inner

    def tp_pieces(x):
        line = [x] + [to_outer(x, d) for d in range(1, outer)]
        pieces = [(owner(d, 0), piece) for d, piece in enumerate(line)]
        for e in range(1, inner):
            pieces += [(owner(d, e), to_inner(piece, e)) for d, piece in enumerate(line)]
        return pieces

    def placed(pieces, count):
        size = pieces[0][1].shape[0]
        whole = jnp.zeros((count * size,) + pieces[0][1].shape[1:], pieces[0][1].dtype)
        for at, piece in pieces:
            whole = lax.dynamic_update_slice_in_dim(whole, piece, at * size, 0)
        return whole

    target_all = placed(tp_pieces(target), tp_count)
    back_all = placed(tp_pieces(out_grad), tp_count)

    target_wide = target.astype(F32)
    root_mean = jnp.sqrt(jnp.mean(target_wide * target_wide, axis=1, keepdims=True) + 1e-06)
    normed = (target_wide / root_mean * norm_gain).astype(BF16)
    block_width = model_width // sp_count

    keys = dot(source, key_weight, ((1,), (0,))).astype(BF16)
    values = dot(source, value_weight, ((1,), (0,))).astype(BF16)

    def pair_of(at):
        return at % outer * inner * local_heads // group_size

    def pair_cols(at):
        start = pair_of(at) * HEAD_DIM
        return jnp.concatenate(
            [lax.dynamic_slice_in_dim(x, start, HEAD_DIM, 1) for x in (keys, values)], axis=1
        )

    line = [pair_cols(outer_at)] + [
        to_outer(pair_cols(outer_at + d), d) for d in range(1, outer)
    ]
    line = jnp.concatenate(line, axis=0)
    target_all, line, normed, root_mean = lax.optimization_barrier(
        (target_all, line, normed, root_mean)
    )
    normed_all = lax.all_gather(normed, ("sp", "tp"), axis=0, tiled=True)
    normed_cols = lax.dynamic_slice_in_dim(normed_all, sp_at * block_width, block_width, 1)
    pairs = jnp.concatenate([line] + [to_inner(line, e) for e in range(1, inner)], axis=0)

    message = project(
        target_all, back_all, norm_gain, query_weight, output_weight, saved_out, log_shift
    )
    grads = None
    query_sum = None
    count = source.shape[0]
    kept = outer * count
    for d in range(sp_count):
        if d + 1 < sp_count:
            following = to_sp(message, 1)
        part, grads, *sent = attend(
            message,
            pairs,
            grads,
            offset,
            local_heads,
            target_all.shape[0],
            kept if d + 1 == sp_count else None,
        )
        if d + 1 < sp_count:
            following, part = lax.optimization_barrier((following, part))
        if d:
            part = to_sp(part, sp_count - d)
        query_sum = part.astype(F32) if query_sum is None else query_sum + part.astype(F32)
        message = following
    query_grad = query_sum.astype(BF16)

    gathered = placed(
        [(sp_at, query_grad)]
        + [((sp_at - d) % sp_count, to_sp(query_grad, d)) for d in range(1, sp_count)],
        sp_count,
    )

    partial = dot(query_grad, query_weight, ((1,), (1,))).astype(BF16)

    def rows_of(at):
        return lax.dynamic_slice_in_dim(partial, at * own_rows, own_rows, 0)

    def line_of(e):
        return jnp.concatenate([rows_of(owner(d, e)) for d in range(outer)], axis=0)

    line = line_of(0).astype(F32)
    for e in range(1, inner):
        line = line + to_inner(line_of(e), inner - e).astype(F32)
    normed_grad = line[:own_rows]
    for d in range(1, outer):
        piece = line[d * own_rows : (d + 1) * own_rows].astype(BF16)
        normed_grad = normed_grad + to_outer(piece, outer - d).astype(F32)

    scaled_grad = normed_grad * norm_gain
    target_grad = (
        scaled_grad / root_mean
        - target_wide * jnp.mean(scaled_grad * target_wide, axis=1, keepdims=True) / root_mean**3
    )

    for e in range(1, inner):
        piece = sent[0][(e - 1) * kept : e * kept]
        grads = grads + to_inner(piece, inner - e).astype(F32)
    grads = grads.astype(BF16)
    combined = []
    for d in range(outer):
        piece = grads[d * count : (d + 1) * count]
        combined.append((pair_of(outer_at + d), to_outer(piece, outer - d) if d else piece))
    source_grad = None
    key_cols, value_cols = [], []
    for p in range(KV_HEADS):
        total = None
        for at, piece in combined:
            piece = jnp.where(at == p, piece.astype(F32), 0.0)
            total = piece if total is None else total + piece
        total = total.astype(BF16)
        key_cols.append(total[:, :HEAD_DIM])
        value_cols.append(total[:, HEAD_DIM:])
    source_grad = dot(jnp.concatenate(key_cols, axis=1), key_weight, ((1,), (1,))) + dot(
        jnp.concatenate(value_cols, axis=1), value_weight, ((1,), (1,))
    )

    query_weight_grad = dot(normed_cols, gathered, ((0,), (0,)))
    return (target_grad, source_grad, query_weight_grad)


def solution(mesh):
    return jax.shard_map(
        shards,
        mesh=mesh,
        in_specs=(
            P(("grp", "sp", "tp"), None),
            P(("grp", "sp", "tp"), None),
            P(),
            P(None, "tp"),
            P(),
            P(),
            P("tp", None),
            P(("grp", "sp"), "tp"),
            P("tp", ("grp", "sp")),
            P(("grp", "sp", "tp"), None),
        ),
        out_specs=(
            P(("grp", "sp", "tp"), None),
            P(("grp", "sp", "tp"), None),
            P(("grp", "sp"), "tp"),
        ),
        check_vma=False,
    )
```

```python
import math

import jax
import jax.numpy as jnp
from jax import lax
from jax.experimental import pallas as pl
from jax.experimental.pallas import tpu as pltpu
from jax.sharding import PartitionSpec as P

HEADS = 16
HEAD_DIM = 128
KV_HEADS = 2
LOG2E = math.log2(math.e)
FACTOR = HEAD_DIM ** (-0.5)
BF16 = jnp.bfloat16
F32 = jnp.float32


def dot(a, b, dims):
    return lax.dot_general(a, b, (dims, ((), ())), preferred_element_type=F32)


def vmem(count):
    return [pl.BlockSpec(memory_space=pltpu.VMEM) for _ in range(count)]


def project_kernel(
    target_ref, back_ref, gain_ref, wq_ref, wo_ref, saved_ref, shift_ref, message_ref
):
    rows = target_ref.shape[0]
    width = wq_ref.shape[1]
    heads = width // HEAD_DIM
    wide = target_ref[...].astype(F32)
    root = jnp.sqrt(jnp.mean(wide * wide, axis=1, keepdims=True) + 1e-06)
    normed = (wide / root * gain_ref[...]).astype(BF16)
    message_ref[:rows, :width] = dot(normed, wq_ref[...], ((1,), (0,))).astype(BF16)
    back = dot(back_ref[...], wo_ref[...], ((1,), (1,))).astype(BF16)
    message_ref[:rows, width:] = back
    products = back.astype(F32) * saved_ref[...].astype(F32)
    ones = jnp.ones((8, HEAD_DIM), F32)
    drops = [
        lax.dot_general(
            ones,
            products[:, h * HEAD_DIM : (h + 1) * HEAD_DIM],
            (((1,), (1,)), ((), ())),
            preferred_element_type=F32,
            precision=lax.Precision.HIGHEST,
        )[:1]
        for h in range(heads)
    ]
    stats = jnp.concatenate([shift_ref[...]] + drops, axis=0)
    high = stats.astype(BF16).astype(F32)
    stats = jnp.concatenate([high, stats - high], axis=0)
    extra = message_ref.shape[0] - rows
    if extra > 4 * heads:
        stats = jnp.concatenate([stats, jnp.zeros((extra - 4 * heads, rows), F32)], axis=0)
    message_ref[rows:, :rows] = stats.astype(BF16)
    if rows < message_ref.shape[1]:
        message_ref[rows:, rows:] = jnp.zeros((extra, message_ref.shape[1] - rows), BF16)


def project(target, back, gain, wq, wo, saved, shift):
    rows, width = target.shape
    heads = wq.shape[1] // HEAD_DIM
    extra = -(-4 * heads // 16) * 16
    return pl.pallas_call(
        project_kernel,
        in_specs=vmem(7),
        out_specs=vmem(1)[0],
        out_shape=jax.ShapeDtypeStruct((rows + extra, 2 * heads * HEAD_DIM), BF16),
        name="project",
    )(target, back, gain.reshape(1, width), wq, wo, saved, shift)


def attend(message, pairs, grads, offset, heads, rows, kept=None):
    source_rows = pairs.shape[0]
    tile = min(source_rows, 256)
    first = grads is None
    last = kept is not None
    width = heads * HEAD_DIM

    def kernel(message_ref, pairs_ref, *rest):
        grads_in = None if first else rest[0]
        outs = rest[0 if first else 1 :]
        part_ref = outs[0]
        parts = [slice(h * HEAD_DIM, (h + 1) * HEAD_DIM) for h in range(heads)]
        queries = jnp.concatenate([message_ref[:rows, p] for p in parts], axis=0)
        backs = jnp.concatenate(
            [message_ref[:rows, width + p.start : width + p.stop] for p in parts], axis=0
        )
        stats = message_ref[rows:, :rows].astype(F32)
        stats = stats[: 2 * heads] + stats[2 * heads : 4 * heads]
        line = lambda at: jnp.concatenate([stats[at + h : at + h + 1] for h in range(heads)], axis=1)
        shifts = (line(0) + offset) * LOG2E
        drops = line(heads)
        total = None
        for at in range(0, source_rows, tile):
            span = slice(at, at + tile)
            keys = pairs_ref[span, :HEAD_DIM]
            values = pairs_ref[span, HEAD_DIM:]
            scores = dot(keys, queries, ((1,), (1,)))
            prob = jnp.exp2(scores * (FACTOR * LOG2E) - shifts)
            prob_grad = dot(values, backs, ((1,), (1,)))
            score_grad = (prob * (prob_grad - drops) * FACTOR).astype(BF16)
            key_part = dot(score_grad, queries, ((1,), (0,)))
            value_part = dot(prob.astype(BF16), backs, ((1,), (0,)))
            if not first:
                key_part = key_part + grads_in[span, :HEAD_DIM]
                value_part = value_part + grads_in[span, HEAD_DIM:]
            if last and at >= kept:
                to, place = outs[2], slice(at - kept, at - kept + tile)
            else:
                to, place = outs[1], span
            to[place, :HEAD_DIM] = key_part.astype(to.dtype)
            to[place, HEAD_DIM:] = value_part.astype(to.dtype)
            share = dot(score_grad, keys, ((0,), (0,)))
            total = share if total is None else total + share
        for h, p in enumerate(parts):
            part_ref[:, p] = total[h * rows : (h + 1) * rows].astype(BF16)

    held = kept if last else source_rows
    shapes = [
        jax.ShapeDtypeStruct((rows, width), BF16),
        jax.ShapeDtypeStruct((held, 2 * HEAD_DIM), F32),
    ]
    if last and kept < source_rows:
        shapes.append(jax.ShapeDtypeStruct((source_rows - kept, 2 * HEAD_DIM), BF16))
    operands = (message, pairs) + (() if first else (grads,))
    return pl.pallas_call(
        kernel,
        in_specs=vmem(len(operands)),
        out_specs=vmem(len(shapes)),
        out_shape=shapes,
        input_output_aliases={} if first or last else {2: 1},
        cost_estimate=pl.CostEstimate(
            flops=10 * rows * width * source_rows,
            transcendentals=rows * heads * source_rows,
            bytes_accessed=8 * source_rows * width,
        ),
        name="attend",
    )(*operands)


def shards(
    target,
    source,
    norm_gain,
    query_weight,
    key_weight,
    value_weight,
    output_weight,
    saved_out,
    log_shift,
    out_grad,
):
    tp_count = lax.axis_size("tp")
    sp_count = lax.axis_size("sp")
    local_heads = query_weight.shape[1] // HEAD_DIM
    group_size = HEADS // KV_HEADS
    inner = 2 if tp_count % 2 == 0 and group_size % (2 * local_heads) == 0 else 1
    outer = tp_count // inner
    tp_at = lax.axis_index("tp")
    sp_at = lax.axis_index("sp")
    outer_at, inner_at = tp_at // inner, tp_at % inner
    offset = math.log(source.shape[0] * tp_count * sp_count)
    own_rows, model_width = target.shape

    def to_outer(x, d):
        pairs = [
            (o * inner + c, (o + d) % outer * inner + c) for o in range(outer) for c in range(inner)
        ]
        return lax.ppermute(x, "tp", pairs)

    def to_inner(x, e):
        pairs = [
            (o * inner + c, o * inner + (c + e) % inner) for o in range(outer) for c in range(inner)
        ]
        return lax.ppermute(x, "tp", pairs)

    def to_sp(x, d):
        return lax.ppermute(x, "sp", [(i, (i + d) % sp_count) for i in range(sp_count)])

    def owner(d, e):
        return (outer_at - d) % outer * inner + (inner_at - e) % inner

    def tp_pieces(x):
        line = [x] + [to_outer(x, d) for d in range(1, outer)]
        pieces = [(owner(d, 0), piece) for d, piece in enumerate(line)]
        for e in range(1, inner):
            pieces += [(owner(d, e), to_inner(piece, e)) for d, piece in enumerate(line)]
        return pieces

    def placed(pieces, count):
        size = pieces[0][1].shape[0]
        whole = jnp.zeros((count * size,) + pieces[0][1].shape[1:], pieces[0][1].dtype)
        for at, piece in pieces:
            whole = lax.dynamic_update_slice_in_dim(whole, piece, at * size, 0)
        return whole

    target_all = placed(tp_pieces(target), tp_count)
    back_all = placed(tp_pieces(out_grad), tp_count)

    target_wide = target.astype(F32)
    root_mean = jnp.sqrt(jnp.mean(target_wide * target_wide, axis=1, keepdims=True) + 1e-06)
    normed = (target_wide / root_mean * norm_gain).astype(BF16)
    block_width = model_width // sp_count

    keys = dot(source, key_weight, ((1,), (0,))).astype(BF16)
    values = dot(source, value_weight, ((1,), (0,))).astype(BF16)

    def pair_of(at):
        return at % outer * inner * local_heads // group_size

    def pair_cols(at):
        start = pair_of(at) * HEAD_DIM
        return jnp.concatenate(
            [lax.dynamic_slice_in_dim(x, start, HEAD_DIM, 1) for x in (keys, values)], axis=1
        )

    line = [pair_cols(outer_at)] + [
        to_outer(pair_cols(outer_at + d), d) for d in range(1, outer)
    ]
    line = jnp.concatenate(line, axis=0)
    target_all, line, normed, root_mean = lax.optimization_barrier(
        (target_all, line, normed, root_mean)
    )

    def normed_block(at):
        return lax.dynamic_slice_in_dim(normed, at % sp_count * block_width, block_width, 1)

    columns = [normed_block(sp_at + d) for d in range(sp_count)]
    columns_at = [(sp_at - d) % sp_count for d in range(sp_count)]
    pieces = None
    pairs = jnp.concatenate([line] + [to_inner(line, e) for e in range(1, inner)], axis=0)

    message = project(
        target_all, back_all, norm_gain, query_weight, output_weight, saved_out, log_shift
    )
    grads = None
    query_sum = None
    count = source.shape[0]
    kept = outer * count
    for d in range(sp_count):
        if d + 1 < sp_count:
            following = to_sp(message, 1)
        part, grads, *sent = attend(
            message,
            pairs,
            grads,
            offset,
            local_heads,
            target_all.shape[0],
            kept if d + 1 == sp_count else None,
        )
        if d + 1 < sp_count:
            held = pieces if pieces is not None else columns
            following, part, held = lax.optimization_barrier((following, part, held))
            if d == 0:
                columns = [held[0]] + [to_sp(held[e], e) for e in range(1, sp_count)]
            elif pieces is None:
                pieces = [x for _, x in tp_pieces(placed(list(zip(columns_at, held)), sp_count))]
            else:
                pieces = held
        if d:
            part = to_sp(part, sp_count - d)
        query_sum = part.astype(F32) if query_sum is None else query_sum + part.astype(F32)
        message = following
    query_grad = query_sum.astype(BF16)

    gathered = placed(
        [(sp_at, query_grad)]
        + [((sp_at - d) % sp_count, to_sp(query_grad, d)) for d in range(1, sp_count)],
        sp_count,
    )

    partial = dot(query_grad, query_weight, ((1,), (1,))).astype(BF16)

    def rows_of(at):
        return lax.dynamic_slice_in_dim(partial, at * own_rows, own_rows, 0)

    def line_of(e):
        return jnp.concatenate([rows_of(owner(d, e)) for d in range(outer)], axis=0)

    line = line_of(0).astype(F32)
    for e in range(1, inner):
        line = line + to_inner(line_of(e), inner - e).astype(F32)
    normed_grad = line[:own_rows]
    for d in range(1, outer):
        piece = line[d * own_rows : (d + 1) * own_rows].astype(BF16)
        normed_grad = normed_grad + to_outer(piece, outer - d).astype(F32)

    scaled_grad = normed_grad * norm_gain
    target_grad = (
        scaled_grad / root_mean
        - target_wide * jnp.mean(scaled_grad * target_wide, axis=1, keepdims=True) / root_mean**3
    )

    for e in range(1, inner):
        piece = sent[0][(e - 1) * kept : e * kept]
        grads = grads + to_inner(piece, inner - e).astype(F32)
    grads = grads.astype(BF16)
    combined = []
    for d in range(outer):
        piece = grads[d * count : (d + 1) * count]
        combined.append((pair_of(outer_at + d), to_outer(piece, outer - d) if d else piece))
    source_grad = None
    key_cols, value_cols = [], []
    for p in range(KV_HEADS):
        total = None
        for at, piece in combined:
            piece = jnp.where(at == p, piece.astype(F32), 0.0)
            total = piece if total is None else total + piece
        total = total.astype(BF16)
        key_cols.append(total[:, :HEAD_DIM])
        value_cols.append(total[:, HEAD_DIM:])
    source_grad = dot(jnp.concatenate(key_cols, axis=1), key_weight, ((1,), (1,))) + dot(
        jnp.concatenate(value_cols, axis=1), value_weight, ((1,), (1,))
    )

    if pieces is None:
        pieces = [x for _, x in tp_pieces(placed(list(zip(columns_at, columns)), sp_count))]
    places = [owner(d, e) for e in range(inner) for d in range(outer)]
    normed_rows = jnp.zeros((sp_count, tp_count, own_rows, block_width), BF16)
    for at, piece in zip(places, pieces):
        piece = piece.reshape(sp_count, 1, own_rows, block_width)
        normed_rows = lax.dynamic_update_slice_in_dim(normed_rows, piece, at, 1)
    query_weight_grad = dot(
        normed_rows.reshape(sp_count * tp_count * own_rows, block_width), gathered, ((0,), (0,))
    )
    return (target_grad, source_grad, query_weight_grad)


def solution(mesh):
    return jax.shard_map(
        shards,
        mesh=mesh,
        in_specs=(
            P(("grp", "sp", "tp"), None),
            P(("grp", "sp", "tp"), None),
            P(),
            P(None, "tp"),
            P(),
            P(),
            P("tp", None),
            P(("grp", "sp"), "tp"),
            P("tp", ("grp", "sp")),
            P(("grp", "sp", "tp"), None),
        ),
        out_specs=(
            P(("grp", "sp", "tp"), None),
            P(("grp", "sp", "tp"), None),
            P(("grp", "sp"), "tp"),
        ),
        check_vma=False,
    )
```
